32 devices in a mesh: ep: 8 (over z, y), tp: 4 (over x, core).
Axes of the slice: x: 2, y: 2, z: 4, core: 2. Of those that a mesh axis runs over, the one named last changes fastest.
Arguments:
- queries: bfloat16 [2048, 768], P('ep', 'tp'), may hold values from -270 to 270
- key_rows: bfloat16 [2048, 256], P('ep', 'tp'), may hold values from -6 to 6
- value_rows: bfloat16 [2048, 256], P('ep', 'tp'), may hold values from -6 to 6
- sink_logits: float32 [12], P('tp'), may hold values from 2 to 6
- out_weight: bfloat16 [768, 2048], P('tp'), may hold values from -0.21875 to 0.21875
- mix_gain: float32 [2048], replicated, may hold values from 0.1 to 1.9
- moe_tokens: bfloat16 [4096, 2048], P(('ep', 'tp')), may hold values from -600 to 600
- moe_gain: float32 [2048], replicated, may hold values from 0.1 to 1.9
- routes: int32 [4096, 2], P(('ep', 'tp')), may hold values from 0 to 7, all different within a row; in each aligned block of 128 rows (0 to 127, 128 to 255, ...) at most 40 rows name the same one
- route_weights: float32 [4096, 2], P(('ep', 'tp')), may hold values from 0.25 to 1.5
- expert_gate: bfloat16 [8, 2048, 3584], P('ep', None, 'tp'), may hold values from -0.125 to 0.125
- expert_up: bfloat16 [8, 2048, 3584], P('ep', None, 'tp'), may hold values from -0.125 to 0.125
- expert_down: bfloat16 [8, 3584, 2048], P('ep', 'tp'), may hold values from -0.09375 to 0.09375
Outputs:
- mixed: bfloat16 [2048, 2048], P(('ep', 'tp'))
- moe_out: bfloat16 [4096, 2048], P(('ep', 'tp'))
The draws below stay inside these ranges and needn't reach their ends.
Inputs may be any that keep to these rules, and one draw needn't show every extreme that they name: `routes`: each row names 2 different experts. In the rows of one device no expert is named more than 40 times, and in every draw some device names some expert exactly 40 times.
All inputs are finite; a program needn't handle non-finite values.
Results may differ from the reference program's by a relative error of at most 0.012.
Values may be sent and summed in bfloat16 or wider, within the bound.
A program may use at most 128 MiB of HBM per device.

```python
import math
import jax
import jax.numpy as jnp
import numpy as np
from jax import lax

D = 2048
FF = 3584
HEADS = 12
KV_HEADS = 4
HDIM = 64
GROUP = 3
WINDOW = 128
TOP = 2
TOK_EP = 256
ROWS_DEV = 128
TOKENS = 2048
ROWS = 4096
EXPERTS = 8
CAP = 40
N_EP = 8
N_TP = 4


def attention_draws(key):
    base = jax.random.fold_in(key, 4242)
    key_part = jnp.clip(jax.random.normal(jax.random.fold_in(base, 1), (TOKENS, KV_HEADS, HDIM), jnp.float32), -6.0, 6.0)
    query_part = jnp.clip(jax.random.normal(jax.random.fold_in(base, 2), (TOKENS, KV_HEADS, GROUP, HDIM), jnp.float32), -6.0, 6.0)
    return (key_part, query_part)


def draw_queries(key, part):
    key_part, query_part = attention_draws(key)
    return query_part.reshape(TOKENS, HEADS * HDIM).astype(jnp.bfloat16)


def draw_key_rows(key, part):
    key_part, query_part = attention_draws(key)
    return key_part.reshape(TOKENS, KV_HEADS * HDIM).astype(jnp.bfloat16)


def draw_moe_tokens(key, part):
    base = jax.random.fold_in(key, 5151)
    tokens_draw = jnp.clip(jax.random.normal(jax.random.fold_in(base, 1), (ROWS, D), jnp.float32), -6.0, 6.0)
    return tokens_draw.astype(jnp.bfloat16)


def block_scale(own_key, shape, shards, least, high):
    def one(dim, shards_of):
        draws = jax.random.uniform(jax.random.fold_in(jax.random.fold_in(own_key, 6), dim), (shards_of,), jnp.float32, least / len(shards), high / len(shards))
        return jnp.repeat(jnp.exp(draws), shape[dim] // shards_of).reshape((-1,) + (1,) * (len(shape) - dim - 1))

    loudness = one(*shards[0])
    for cut in shards[1:]:
        loudness = loudness * one(*cut)
    return loudness


def assign_block(stream_key, own, number, rows, count, top, bound, skew):
    sequence = jax.random.permutation(stream_key, count)
    heavy_load, common = load_shares(count, rows * top, bound, skew, True), load_shares(count, rows * top, bound, skew, False)
    places = jnp.arange(count)

    def named(lengths, turn):
        used = int((lengths > 0).sum())
        fixed = max(1, used // 4)
        moved = fixed + (places - fixed + turn * (used - fixed)) % max(1, count - fixed)
        return jnp.zeros((count,), jnp.int32).at[sequence[jnp.where(places < fixed, places, moved)]].set(jnp.asarray(lengths, jnp.int32))

    lengths = jnp.where(number % 4 == 0, named(heavy_load, number // 4), named(common, number - number // 4 - 1))
    mixed = jax.random.permutation(jax.random.fold_in(own, 3), count)
    source_of, receiver = mixed[0:count // 2 * 2:2], mixed[1:count // 2 * 2:2]
    margin = jnp.minimum(lengths[source_of] - 1, bound - lengths[receiver]) // 2
    margin = jnp.where((source_of == sequence[0]) | (receiver == sequence[0]) | (lengths[receiver] == 0), 0, jnp.maximum(margin, 0))
    moved = jax.random.randint(jax.random.fold_in(own, 4), (count // 2,), 0, 1 << 20) % (margin + 1)
    lengths = lengths.at[source_of].add(-moved).at[receiver].add(moved)
    items = jnp.searchsorted(jnp.cumsum(lengths), jnp.arange(rows * top), side="right").astype(jnp.int32)
    grid = items.reshape(top, rows).T
    grid = grid[jax.random.permutation(jax.random.fold_in(own, 1), rows)]
    turn = jax.random.randint(jax.random.fold_in(own, 2), (rows, 1), 0, top)
    return jnp.take_along_axis(grid, (jnp.arange(top)[None, :] + turn) % top, axis=1)


def load_shares(count, total, reach, skew, full):
    portions = [(1 << 20) // math.isqrt(standing ** skew) + 1 for standing in range(1, count + 1)]
    largest = reach if full else min(reach, max(-(-total // count), total * portions[0] // sum(portions)))
    least = 1 if total - largest >= count - 1 else 0
    given, rest = [largest] + [least] * (count - 1), total - largest - least * (count - 1)
    while rest > 0:
        candidates = [i for i in range(1, count) if given[i] < largest] or [i for i in range(1, count) if given[i] < reach]
        mass, remaining = sum([portions[i] for i in candidates]), rest
        for i in candidates:
            extra = min(reach - given[i], max(1, remaining * portions[i] // mass), rest)
            given[i] = given[i] + extra
            rest = rest - extra
    return np.array(given)


def gaussian(stream_key, dims, width, most, cuts=(), held_as=jnp.bfloat16):
    result = jax.random.normal(stream_key, dims, jnp.float32) * width
    if len(cuts) > 0:
        result = block_scale(stream_key, dims, cuts, -0.22, 0.18) * result
    return jnp.clip(result, min=-most, max=most).astype(held_as)


def setup_inputs(seed: int = 0) -> dict:
    arg_keys = jax.random.split(jax.random.key(seed), 14)
    queries = draw_queries(jax.random.fold_in(arg_keys[13], 71), 0)
    key_rows = draw_key_rows(jax.random.fold_in(arg_keys[13], 71), 0)
    value_rows = gaussian(arg_keys[2], (TOKENS, KV_HEADS * HDIM), 1.0, 6.0, ((0, 8), (1, 4)))
    sink_logits = jnp.clip(2.0 + 4.0 * jax.random.uniform(arg_keys[3], (HEADS,), jnp.float32) ** block_scale(arg_keys[3], (HEADS,), ((0, 4),), -0.2, 0.2), 2.0, 6.0)
    out_weight = gaussian(arg_keys[4], (HEADS * HDIM, D), (HEADS * HDIM) ** -0.5, 0.21875, ((0, 4),))
    mix_gain = jnp.clip(1.0 + 0.18 * jax.random.normal(arg_keys[5], (D,), jnp.float32), 0.1, 1.9)
    moe_tokens = draw_moe_tokens(jax.random.fold_in(arg_keys[13], 71), 0)
    moe_gain = jnp.clip(1.0 + 0.18 * jax.random.normal(arg_keys[7], (D,), jnp.float32), 0.1, 1.9)
    routes_keys = jax.random.split(jax.random.fold_in(arg_keys[8], 1), ROWS // ROWS_DEV)
    routes_turns = jax.random.permutation(jax.random.fold_in(arg_keys[8], 3), ROWS // ROWS_DEV)
    routes = jax.vmap(lambda own, number: assign_block(jax.random.fold_in(arg_keys[8], 2), own, number, ROWS_DEV, EXPERTS, TOP, CAP, 0))(routes_keys, routes_turns).reshape((ROWS, TOP))
    route_weights = jnp.clip(jnp.exp(math.log(1.5) - 1.7917595 * jax.random.uniform(arg_keys[9], (ROWS, TOP), jnp.float32) ** block_scale(arg_keys[9], (ROWS, TOP), ((0, 32),), -0.2, 0.2)), 0.25, 1.5)
    expert_gate = gaussian(arg_keys[10], (EXPERTS, D, FF), D ** -0.5, 0.125, ((0, 8), (2, 4)))
    expert_up = gaussian(arg_keys[11], (EXPERTS, D, FF), D ** -0.5, 0.125, ((0, 8), (2, 4)))
    expert_down = gaussian(arg_keys[12], (EXPERTS, FF, D), FF ** -0.5, 0.09375, ((0, 8), (1, 4)))
    return dict(queries=queries, key_rows=key_rows, value_rows=value_rows, sink_logits=sink_logits, out_weight=out_weight, mix_gain=mix_gain, moe_tokens=moe_tokens, moe_gain=moe_gain, routes=routes, route_weights=route_weights, expert_gate=expert_gate, expert_up=expert_up, expert_down=expert_down)


norm_eps = 1e-06
masked_value = -1e+30

def rms_scale(rows_in, gain):
    squares = lax.optimization_barrier(jnp.mean(rows_in * rows_in, axis=-1, keepdims=True))
    return rows_in * lax.rsqrt(squares + norm_eps) * gain

def reference(queries, key_rows, value_rows, sink_logits, out_weight, mix_gain, moe_tokens, moe_gain, routes, route_weights, expert_gate, expert_up, expert_down):
    head_cols = KV_HEADS * HDIM
    padded_keys = jnp.concatenate([jnp.zeros((WINDOW, head_cols), jnp.bfloat16), key_rows], axis=0)
    padded_values = jnp.concatenate([jnp.zeros((WINDOW, head_cols), jnp.bfloat16), value_rows], axis=0)

    def attend_block(block_index):
        first_row = (block_index * TOK_EP).astype(jnp.int32)
        block_queries = lax.dynamic_slice_in_dim(queries, first_row, TOK_EP, 0)
        block_keys = lax.dynamic_slice_in_dim(padded_keys, first_row, TOK_EP + WINDOW, 0)
        block_values = lax.dynamic_slice_in_dim(padded_values, first_row, TOK_EP + WINDOW, 0)
        query_pos = first_row + jnp.arange(TOK_EP, dtype=jnp.int32)
        key_pos = first_row - WINDOW + jnp.arange(TOK_EP + WINDOW, dtype=jnp.int32)
        distance = query_pos[:, None] - key_pos[None, :]
        allowed = (distance >= 0) & (distance < WINDOW) & (key_pos >= 0)[None, :]
        grouped = block_queries.reshape(TOK_EP, KV_HEADS, GROUP, HDIM).astype(jnp.float32)
        keys_f = block_keys.reshape(TOK_EP + WINDOW, KV_HEADS, HDIM).astype(jnp.float32)
        values_f = block_values.reshape(TOK_EP + WINDOW, KV_HEADS, HDIM).astype(jnp.float32)
        scores = jnp.einsum('qkgd,jkd->kgqj', grouped, keys_f) * HDIM ** (-0.5)
        logits = jnp.where(allowed, scores, masked_value)
        sink_logit = sink_logits.reshape(KV_HEADS, GROUP)[:, :, None, None]
        top_value = jnp.maximum(lax.optimization_barrier(jnp.max(logits, axis=-1, keepdims=True)), sink_logit)
        exponent = jnp.exp(logits - top_value)
        denominator = lax.optimization_barrier(jnp.sum(exponent, axis=-1, keepdims=True)) + jnp.exp(sink_logit - top_value)
        probs = (exponent / denominator).astype(jnp.bfloat16)
        attended = jnp.einsum('kgqj,jkd->qkgd', probs.astype(jnp.float32), values_f)
        return attended.astype(jnp.bfloat16).reshape(TOK_EP, HEADS * HDIM)
    attended = lax.map(attend_block, jnp.arange(N_EP, dtype=jnp.int32)).reshape(TOKENS, HEADS * HDIM)
    group_cols = HEADS * HDIM // N_TP
    projected = jnp.zeros((TOKENS, D), jnp.float32)
    for group_index in range(N_TP):
        lower = group_index * group_cols
        partial_value = jnp.dot(attended[:, lower:lower + group_cols], out_weight[lower:lower + group_cols], preferred_element_type=jnp.float32).astype(jnp.bfloat16)
        partial_value = lax.optimization_barrier(partial_value)
        projected = projected + partial_value.astype(jnp.float32)
    mixed = rms_scale(projected, mix_gain).astype(jnp.bfloat16)
    normed = rms_scale(moe_tokens.astype(jnp.float32), moe_gain).astype(jnp.bfloat16)
    slot_limit = N_EP * N_TP * CAP
    ff_block = FF // N_TP

    def expert_step(accumulated, inputs):
        gate_weight, up_weight, down_weight, expert_id = inputs
        chosen = routes == expert_id
        token_weight = lax.optimization_barrier(jnp.sum(jnp.where(chosen, route_weights, jnp.zeros_like(route_weights)), axis=1))
        member = jnp.any(chosen, axis=1)
        token_index = jnp.nonzero(member, size=slot_limit, fill_value=0)[0].astype(jnp.int32)
        valid_slot = jnp.arange(slot_limit, dtype=jnp.int32) < jnp.sum(member.astype(jnp.int32))
        slot_rows = normed[token_index]
        gate_value = jnp.dot(slot_rows, gate_weight, preferred_element_type=jnp.float32)
        up_value = jnp.dot(slot_rows, up_weight, preferred_element_type=jnp.float32)
        hidden = (jax.nn.silu(gate_value) * up_value).astype(jnp.bfloat16)
        summed = jnp.zeros((slot_limit, D), jnp.float32)
        for block_index in range(N_TP):
            lower = block_index * ff_block
            partial_value = jnp.dot(hidden[:, lower:lower + ff_block], down_weight[lower:lower + ff_block], preferred_element_type=jnp.float32).astype(jnp.bfloat16)
            partial_value = lax.optimization_barrier(partial_value)
            summed = summed + partial_value.astype(jnp.float32)
        expert_out = lax.optimization_barrier(summed.astype(jnp.bfloat16))
        row_weight = jnp.where(valid_slot, token_weight[token_index], jnp.zeros_like(token_weight[token_index]))
        accumulated = accumulated.at[token_index].add(row_weight[:, None] * expert_out.astype(jnp.float32))
        return (accumulated, None)
    combined, _ = lax.scan(expert_step, jnp.zeros((ROWS, D), jnp.float32), (expert_gate, expert_up, expert_down, jnp.arange(EXPERTS, dtype=jnp.int32)))
    return (mixed, combined.astype(jnp.bfloat16))
```

```python
import functools

import jax
import jax.numpy as jnp
from jax import lax
from jax.experimental import pallas as pl
from jax.experimental.pallas import tpu as pltpu
from jax.sharding import PartitionSpec as P

HDIM = 64
WINDOW = 128
MESH = pl.DeviceIdType.MESH


norm_eps = 1e-06
masked_value = -1e30


def rms_scale(rows_in, gain):
    squares = jnp.mean(rows_in * rows_in, axis=-1, keepdims=True)
    return rows_in * lax.rsqrt(squares + norm_eps) * gain


def slot_places(route_rows, experts, capacity):
    tok_rows, top_count = route_rows.shape
    flat_routes = route_rows.reshape(tok_rows * top_count)
    onehot = (flat_routes[:, None] == jnp.arange(experts, dtype=jnp.int32)[None, :]).astype(jnp.int32)
    earlier = jnp.cumsum(onehot, axis=0) - onehot
    slot_rank = jnp.sum(earlier * onehot, axis=1)
    return (flat_routes * capacity + slot_rank).reshape(tok_rows, top_count)


def far_first(n):
    return sorted(range(1, n), key=lambda k: -min(k, n - k))


def places():
    ep, tp = lax.axis_index("ep"), lax.axis_index("tp")
    pair = tp + 1 - 2 * lax.rem(tp, 2)
    cross = lax.rem(tp + 2, 4)
    return ep, tp, pair, cross


def enter(n, ep, tp, pair, cross):
    barrier = pltpu.get_barrier_semaphore()
    for k in range(1, n):
        pl.semaphore_signal(barrier, inc=1, device_id=(lax.rem(ep + k, n), tp), device_id_type=MESH)
    for other in (pair, cross):
        pl.semaphore_signal(barrier, inc=1, device_id=(ep, other), device_id_type=MESH)
    pl.semaphore_wait(barrier, n + 1)


def send(src, dst, send_sem, recv_sem, where):
    copy = pltpu.make_async_remote_copy(
        src_ref=src, dst_ref=dst, send_sem=send_sem, recv_sem=recv_sem,
        device_id=where, device_id_type=MESH,
    )
    copy.start()
    return copy


def dispatch_kernel(
    n, out_ref, q_ref, kv_ref, sink_ref, w_ref, gain_ref,
    slots, mixed_ref,
    kv_prev, part, mix_in, mix_sum, mix_x,
    send_d, recv_d, send_p, recv_p, send_x, recv_x, send_q, recv_q, send_m, recv_m,
):
    ep, tp, pair, cross = places()
    diag = lax.rem(pair + 2, 4)
    enter(n, ep, tp, pair, cross)
    tok_rows = kv_ref.shape[0]
    group_size = q_ref.shape[0]
    copies = []
    halo = send(
        kv_ref.at[pl.ds(tok_rows - WINDOW, WINDOW)], kv_prev,
        send_m.at[0], recv_m.at[0], (lax.rem(ep + 1, n), tp),
    )
    order = far_first(n)
    direct = {}
    own = out_ref.at[ep]
    crossed = {0: send(own, slots.at[2, 0], send_x.at[0], recv_x.at[0], (ep, cross))}
    for k in order:
        to = lax.rem(ep + k, n)
        direct[k] = send(out_ref.at[to], slots.at[0, k], send_d.at[k], recv_d.at[k], (to, tp))
    copies.append(send(own, slots.at[1, 0], send_p.at[0], recv_p.at[0], (ep, pair)))
    slots[0, 0] = out_ref[ep]

    halo.wait()
    rows = tok_rows + WINDOW
    kv = jnp.concatenate([kv_prev[...], kv_ref[...]], axis=0)
    row = lax.broadcasted_iota(jnp.int32, (tok_rows, rows), 0)
    col = lax.broadcasted_iota(jnp.int32, (tok_rows, rows), 1)
    distance = row - (col - WINDOW)
    key_pos = ep * tok_rows - WINDOW + col
    allowed = (distance >= 0) & (distance < WINDOW) & (key_pos >= 0)
    heads = []
    for g in range(group_size):
        scores = lax.dot_general(
            q_ref[g], kv, (((1,), (1,)), ((), ())), preferred_element_type=jnp.float32
        ) * HDIM ** (-0.5)
        logits = jnp.where(allowed, scores, masked_value)
        sink = sink_ref[g : g + 1, 0:1]
        top = jnp.maximum(jnp.max(logits, axis=-1, keepdims=True), sink)
        exponent = jnp.exp(logits - top)
        denominator = jnp.sum(exponent, axis=-1, keepdims=True) + jnp.exp(sink - top)
        probs = (exponent / denominator).astype(jnp.bfloat16)
        heads.append(jnp.dot(probs, kv, preferred_element_type=jnp.float32).astype(jnp.bfloat16))
    block = tok_rows // 4
    for b in range(4):
        total = None
        for g in range(group_size):
            term = jnp.dot(
                heads[g][b * block : (b + 1) * block], w_ref[g], preferred_element_type=jnp.float32
            )
            total = term if total is None else total + term
        part[b] = total.astype(jnp.bfloat16)
    to_sum = send(part.at[diag], mix_in.at[1], send_m.at[1], recv_m.at[1], (ep, pair))
    to_own = send(part.at[pair], mix_in.at[0], send_m.at[2], recv_m.at[2], (ep, pair))
    to_sum.wait()
    mix_sum[...] = (part[cross].astype(jnp.float32) + mix_in[1].astype(jnp.float32)).astype(jnp.bfloat16)
    over_x = send(mix_sum, mix_x, send_m.at[3], recv_m.at[3], (ep, cross))

    pending = [0]
    for k in order:
        direct[k].wait_recv()
        crossed[k] = send(slots.at[0, k], slots.at[2, k], send_x.at[k], recv_x.at[k], (ep, cross))
        copies.append(send(slots.at[0, k], slots.at[1, k], send_p.at[k], recv_p.at[k], (ep, pair)))
        pending.append(k)
    diagonal = []
    for i, k in enumerate(pending):
        crossed[k].wait_recv()
        diagonal.append(send(slots.at[2, k], slots.at[3, k], send_q.at[k], recv_q.at[k], (ep, pair)))
        if i == 1 or n == 1:
            to_own.wait()
            over_x.wait()
            projected = (
                part[tp].astype(jnp.float32) + mix_in[0].astype(jnp.float32) + mix_x[...].astype(jnp.float32)
            )
            mixed_ref[...] = rms_scale(projected, gain_ref[...]).astype(jnp.bfloat16)
    for copy in copies + diagonal:
        copy.wait()
    for k in order:
        direct[k].wait_send()
    for k in pending:
        crossed[k].wait_send()


def dispatch(outgoing, queries, kv, sinks, weight, gain):
    n, capacity, width = outgoing.shape
    tok_rows = kv.shape[0]
    block = tok_rows // 4
    vmem = pl.BlockSpec(memory_space=pltpu.VMEM)
    sems = pltpu.SemaphoreType.DMA
    return pl.pallas_call(
        functools.partial(dispatch_kernel, n),
        out_shape=(
            jax.ShapeDtypeStruct((4, n, capacity, width), jnp.bfloat16),
            jax.ShapeDtypeStruct((block, width), jnp.bfloat16),
        ),
        in_specs=[vmem] * 6,
        out_specs=(vmem, vmem),
        scratch_shapes=[
            pltpu.VMEM((WINDOW, kv.shape[1]), jnp.bfloat16),
            pltpu.VMEM((4, block, width), jnp.bfloat16),
            pltpu.VMEM((2, block, width), jnp.bfloat16),
            pltpu.VMEM((block, width), jnp.bfloat16),
            pltpu.VMEM((block, width), jnp.bfloat16),
        ]
        + [sems((n,))] * 8
        + [sems((4,))] * 2,
        compiler_params=pltpu.CompilerParams(collective_id=0, has_side_effects=True),
    )(outgoing, queries, kv, sinks, weight, gain)


def combine_kernel(
    n, y_ref, ret, pair_in, cross_out, cross_in, back_out,
    send_a, recv_a, send_b, recv_b, send_x, recv_x, send_r, recv_r,
):
    ep, tp, pair, cross = places()
    enter(n, ep, tp, pair, cross)
    order = far_first(n) + [0]
    first, second, crossed, back = {}, {}, {}, {}
    for k in order:
        first[k] = send(y_ref.at[3, k], pair_in.at[1, k], send_a.at[k], recv_a.at[k], (ep, pair))
    for k in order:
        second[k] = send(y_ref.at[1, k], pair_in.at[0, k], send_b.at[k], recv_b.at[k], (ep, pair))
    for k in order:
        first[k].wait_recv()
        cross_out[k] = (
            y_ref[2, k].astype(jnp.float32) + pair_in[1, k].astype(jnp.float32)
        ).astype(jnp.bfloat16)
        crossed[k] = send(cross_out.at[k], cross_in.at[k], send_x.at[k], recv_x.at[k], (ep, cross))
    for k in order:
        second[k].wait_recv()
        crossed[k].wait_recv()
        total = (
            y_ref[0, k].astype(jnp.float32)
            + pair_in[0, k].astype(jnp.float32)
            + cross_in[k].astype(jnp.float32)
        ).astype(jnp.bfloat16)
        if k == 0:
            ret[ep] = total
        else:
            back_out[k] = total
            to = lax.rem(ep + n - k, n)
            back[k] = send(back_out.at[k], ret.at[ep], send_r.at[k], recv_r.at[k], (to, tp))
    for k in order:
        if k:
            pltpu.make_async_remote_copy(
                src_ref=back_out.at[k], dst_ref=ret.at[lax.rem(ep + k, n)],
                send_sem=send_r.at[k], recv_sem=recv_r.at[k],
                device_id=(lax.rem(ep + n - k, n), tp), device_id_type=MESH,
            ).wait()
    for k in order:
        first[k].wait_send()
        second[k].wait_send()
        crossed[k].wait_send()


def combine(partial_rows):
    _, n, capacity, width = partial_rows.shape
    vmem = pl.BlockSpec(memory_space=pltpu.VMEM)
    sems = pltpu.SemaphoreType.DMA
    blocks = pltpu.VMEM((n, capacity, width), jnp.bfloat16)
    return pl.pallas_call(
        functools.partial(combine_kernel, n),
        out_shape=jax.ShapeDtypeStruct((n, capacity, width), jnp.bfloat16),
        in_specs=[vmem],
        out_specs=vmem,
        scratch_shapes=[pltpu.VMEM((2, n, capacity, width), jnp.bfloat16), blocks, blocks, blocks]
        + [sems((n,))] * 8,
        compiler_params=pltpu.CompilerParams(collective_id=1, has_side_effects=True),
    )(partial_rows)


def shards(
    queries,
    key_rows,
    value_rows,
    sink_logits,
    out_weight,
    mix_gain,
    moe_tokens,
    moe_gain,
    routes,
    route_weights,
    expert_gate,
    expert_up,
    expert_down,
):
    tok_rows, width = moe_tokens.shape
    top_count = routes.shape[1]
    experts = lax.axis_size("ep")
    capacity = tok_rows * top_count * 5 // (4 * experts)
    slots = capacity * experts

    normed = rms_scale(moe_tokens.astype(jnp.float32), moe_gain).astype(jnp.bfloat16)
    slot_place = slot_places(routes, experts, capacity)
    targets = jnp.arange(slots, dtype=jnp.int32)
    hits = (slot_place[None, :, :] == targets[:, None, None]).astype(jnp.float32)
    select_rows = jnp.sum(hits, axis=2).astype(jnp.bfloat16)
    outgoing = jnp.dot(select_rows, normed, preferred_element_type=jnp.float32)
    outgoing = outgoing.astype(jnp.bfloat16).reshape(experts, capacity, width)

    group_size = queries.shape[1] // HDIM
    q = jnp.transpose(queries.reshape(-1, group_size, HDIM), (1, 0, 2))
    q = jnp.pad(q, ((0, 0), (0, 0), (0, HDIM)))
    kv = jnp.concatenate([key_rows, value_rows], axis=1)
    weight = jnp.pad(out_weight.reshape(group_size, HDIM, width), ((0, 0), (HDIM, 0), (0, 0)))
    sinks = jnp.broadcast_to(sink_logits[:, None], (group_size, 128))
    slot_rows, mixed = dispatch(outgoing, q, kv, sinks, weight, mix_gain[None])

    slot_rows = slot_rows.reshape(4 * slots, width)
    gate_value = jnp.dot(slot_rows, expert_gate[0], preferred_element_type=jnp.float32)
    up_value = jnp.dot(slot_rows, expert_up[0], preferred_element_type=jnp.float32)
    hidden = (jax.nn.silu(gate_value) * up_value).astype(jnp.bfloat16)
    blocks = jnp.dot(hidden, expert_down[0], preferred_element_type=jnp.float32).astype(jnp.bfloat16)
    returned = combine(blocks.reshape(4, experts, capacity, width)).reshape(slots, width)

    spots = slot_place[:, :, None] == targets[None, None, :]
    spread = jnp.sum(jnp.where(spots, route_weights[:, :, None], 0.0), axis=1)
    high = spread.astype(jnp.bfloat16)
    low = (spread - high.astype(jnp.float32)).astype(jnp.bfloat16)
    combined = jnp.dot(high, returned, preferred_element_type=jnp.float32) + jnp.dot(
        low, returned, preferred_element_type=jnp.float32
    )
    return (mixed, combined.astype(jnp.bfloat16))


def solution(mesh):
    return jax.shard_map(
        shards,
        mesh=mesh,
        in_specs=(
            P("ep", "tp"),
            P("ep", "tp"),
            P("ep", "tp"),
            P("tp"),
            P("tp", None),
            P(),
            P(("ep", "tp"), None),
            P(),
            P(("ep", "tp"), None),
            P(("ep", "tp"), None),
            P("ep", None, "tp"),
            P("ep", None, "tp"),
            P("ep", "tp", None),
        ),
        out_specs=(P(("ep", "tp"), None), P(("ep", "tp"), None)),
        check_vma=False,
    )
```

```python
import functools

import jax
import jax.numpy as jnp
from jax import lax
from jax.experimental import pallas as pl
from jax.experimental.pallas import tpu as pltpu
from jax.sharding import PartitionSpec as P

HDIM = 64
WINDOW = 128
MESH = pl.DeviceIdType.MESH


norm_eps = 1e-06
masked_value = -1e30


def rms_scale(rows_in, gain):
    squares = jnp.mean(rows_in * rows_in, axis=-1, keepdims=True)
    return rows_in * lax.rsqrt(squares + norm_eps) * gain


def slot_places(route_rows, experts, capacity):
    tok_rows, top_count = route_rows.shape
    flat_routes = route_rows.reshape(tok_rows * top_count)
    onehot = (flat_routes[:, None] == jnp.arange(experts, dtype=jnp.int32)[None, :]).astype(jnp.int32)
    earlier = jnp.cumsum(onehot, axis=0) - onehot
    slot_rank = jnp.sum(earlier * onehot, axis=1)
    return (flat_routes * capacity + slot_rank).reshape(tok_rows, top_count)


def far_first(n):
    return sorted(range(1, n), key=lambda k: -min(k, n - k))


def places():
    ep, tp = lax.axis_index("ep"), lax.axis_index("tp")
    pair = tp + 1 - 2 * lax.rem(tp, 2)
    cross = lax.rem(tp + 2, 4)
    return ep, tp, pair, cross


def enter(n, ep, tp, pair, cross):
    barrier = pltpu.get_barrier_semaphore()
    for k in range(1, n):
        pl.semaphore_signal(barrier, inc=1, device_id=(lax.rem(ep + k, n), tp), device_id_type=MESH)
    for other in (pair, cross):
        pl.semaphore_signal(barrier, inc=1, device_id=(ep, other), device_id_type=MESH)
    pl.semaphore_wait(barrier, n + 1)


def send(src, dst, send_sem, recv_sem, where):
    copy = pltpu.make_async_remote_copy(
        src_ref=src, dst_ref=dst, send_sem=send_sem, recv_sem=recv_sem,
        device_id=where, device_id_type=MESH,
    )
    copy.start()
    return copy


def dispatch_kernel(
    n, out_ref, q_ref, kv_ref, sink_ref, w_ref, gain_ref,
    slots, mixed_ref,
    kv_prev, part, mix_in, mix_sum, mix_x,
    send_d, recv_d, send_p, recv_p, send_x, recv_x, send_q, recv_q, send_m, recv_m,
):
    ep, tp, pair, cross = places()
    diag = lax.rem(pair + 2, 4)
    enter(n, ep, tp, pair, cross)
    tok_rows = kv_ref.shape[0]
    group_size = q_ref.shape[0]
    copies = []
    halo = send(
        kv_ref.at[pl.ds(tok_rows - WINDOW, WINDOW)], kv_prev,
        send_m.at[0], recv_m.at[0], (lax.rem(ep + 1, n), tp),
    )
    order = far_first(n)
    direct = {}
    own = out_ref.at[ep]
    crossed = {0: send(own, slots.at[2, 0], send_x.at[0], recv_x.at[0], (ep, cross))}
    for k in order:
        to = lax.rem(ep + k, n)
        direct[k] = send(out_ref.at[to], slots.at[0, k], send_d.at[k], recv_d.at[k], (to, tp))
    copies.append(send(own, slots.at[1, 0], send_p.at[0], recv_p.at[0], (ep, pair)))
    slots[0, 0] = out_ref[ep]

    halo.wait()
    rows = tok_rows + WINDOW
    kv = jnp.concatenate([kv_prev[...], kv_ref[...]], axis=0)
    row = lax.broadcasted_iota(jnp.int32, (tok_rows, rows), 0)
    col = lax.broadcasted_iota(jnp.int32, (tok_rows, rows), 1)
    distance = row - (col - WINDOW)
    key_pos = ep * tok_rows - WINDOW + col
    allowed = (distance >= 0) & (distance < WINDOW) & (key_pos >= 0)
    heads = []

    def attend(g):
        scores = lax.dot_general(
            q_ref[g], kv, (((1,), (1,)), ((), ())), preferred_element_type=jnp.float32
        ) * HDIM ** (-0.5)
        logits = jnp.where(allowed, scores, masked_value)
        sink = sink_ref[g : g + 1, 0:1]
        top = jnp.maximum(jnp.max(logits, axis=-1, keepdims=True), sink)
        exponent = jnp.exp(logits - top)
        denominator = jnp.sum(exponent, axis=-1, keepdims=True) + jnp.exp(sink - top)
        probs = (exponent / denominator).astype(jnp.bfloat16)
        heads.append(jnp.dot(probs, kv, preferred_element_type=jnp.float32).astype(jnp.bfloat16))

    block = tok_rows // 4
    mixing = {}

    def project():
        for b in range(4):
            total = None
            for g in range(group_size):
                term = jnp.dot(
                    heads[g][b * block : (b + 1) * block], w_ref[g], preferred_element_type=jnp.float32
                )
                total = term if total is None else total + term
            part[b] = total.astype(jnp.bfloat16)
        mixing["sum"] = send(part.at[diag], mix_in.at[1], send_m.at[1], recv_m.at[1], (ep, pair))
        mixing["own"] = send(part.at[pair], mix_in.at[0], send_m.at[2], recv_m.at[2], (ep, pair))

    def cross_part():
        mixing["sum"].wait()
        mix_sum[...] = (part[cross].astype(jnp.float32) + mix_in[1].astype(jnp.float32)).astype(jnp.bfloat16)
        mixing["x"] = send(mix_sum, mix_x, send_m.at[3], recv_m.at[3], (ep, cross))

    pieces = [functools.partial(attend, g) for g in range(group_size)] + [project, cross_part]

    pending = [0]
    for k in order:
        direct[k].wait_recv()
        crossed[k] = send(slots.at[0, k], slots.at[2, k], send_x.at[k], recv_x.at[k], (ep, cross))
        copies.append(send(slots.at[0, k], slots.at[1, k], send_p.at[k], recv_p.at[k], (ep, pair)))
        pending.append(k)
        if pieces:
            pieces.pop(0)()
    for piece in pieces:
        piece()
    diagonal = []
    for i, k in enumerate(pending):
        crossed[k].wait_recv()
        diagonal.append(send(slots.at[2, k], slots.at[3, k], send_q.at[k], recv_q.at[k], (ep, pair)))
        if i == 1 or n == 1:
            mixing["own"].wait()
            mixing["x"].wait()
            projected = (
                part[tp].astype(jnp.float32) + mix_in[0].astype(jnp.float32) + mix_x[...].astype(jnp.float32)
            )
            mixed_ref[...] = rms_scale(projected, gain_ref[...]).astype(jnp.bfloat16)
    for copy in copies + diagonal:
        copy.wait()
    for k in order:
        direct[k].wait_send()
    for k in pending:
        crossed[k].wait_send()


def dispatch(outgoing, queries, kv, sinks, weight, gain):
    n, capacity, width = outgoing.shape
    tok_rows = kv.shape[0]
    block = tok_rows // 4
    vmem = pl.BlockSpec(memory_space=pltpu.VMEM)
    sems = pltpu.SemaphoreType.DMA
    return pl.pallas_call(
        functools.partial(dispatch_kernel, n),
        out_shape=(
            jax.ShapeDtypeStruct((4, n, capacity, width), jnp.bfloat16),
            jax.ShapeDtypeStruct((block, width), jnp.bfloat16),
        ),
        in_specs=[vmem] * 6,
        out_specs=(vmem, vmem),
        scratch_shapes=[
            pltpu.VMEM((WINDOW, kv.shape[1]), jnp.bfloat16),
            pltpu.VMEM((4, block, width), jnp.bfloat16),
            pltpu.VMEM((2, block, width), jnp.bfloat16),
            pltpu.VMEM((block, width), jnp.bfloat16),
            pltpu.VMEM((block, width), jnp.bfloat16),
        ]
        + [sems((n,))] * 8
        + [sems((4,))] * 2,
        compiler_params=pltpu.CompilerParams(collective_id=0, has_side_effects=True),
    )(outgoing, queries, kv, sinks, weight, gain)


def combine_kernel(
    n, h_ref, down_ref, ret, y_ref, pair_in, cross_out, cross_in, back_out,
    send_a, recv_a, send_b, recv_b, send_x, recv_x, send_r, recv_r,
):
    ep, tp, pair, cross = places()
    enter(n, ep, tp, pair, cross)
    order = far_first(n) + [0]
    capacity, width = ret.shape[1:]
    tile = width // 4
    first, second, crossed, back = {}, {}, {}, {}

    def down(r):
        for c in range(0, width, tile):
            product = jnp.dot(
                h_ref[r], down_ref[:, c : c + tile], preferred_element_type=jnp.float32
            ).astype(jnp.bfloat16)
            for k in range(n):
                y_ref[r, k, :, c : c + tile] = product[k * capacity : (k + 1) * capacity]

    down(3)
    for k in order:
        first[k] = send(y_ref.at[3, k], pair_in.at[1, k], send_a.at[k], recv_a.at[k], (ep, pair))
    down(2)
    for k in order:
        first[k].wait_recv()
        cross_out[k] = (
            y_ref[2, k].astype(jnp.float32) + pair_in[1, k].astype(jnp.float32)
        ).astype(jnp.bfloat16)
        crossed[k] = send(cross_out.at[k], cross_in.at[k], send_x.at[k], recv_x.at[k], (ep, cross))
    down(1)
    for k in order:
        second[k] = send(y_ref.at[1, k], pair_in.at[0, k], send_b.at[k], recv_b.at[k], (ep, pair))
    down(0)
    for k in order:
        second[k].wait_recv()
        crossed[k].wait_recv()
        total = (
            y_ref[0, k].astype(jnp.float32)
            + pair_in[0, k].astype(jnp.float32)
            + cross_in[k].astype(jnp.float32)
        ).astype(jnp.bfloat16)
        if k == 0:
            ret[ep] = total
        else:
            back_out[k] = total
            to = lax.rem(ep + n - k, n)
            back[k] = send(back_out.at[k], ret.at[ep], send_r.at[k], recv_r.at[k], (to, tp))
    for k in order:
        if k:
            pltpu.make_async_remote_copy(
                src_ref=back_out.at[k], dst_ref=ret.at[lax.rem(ep + k, n)],
                send_sem=send_r.at[k], recv_sem=recv_r.at[k],
                device_id=(lax.rem(ep + n - k, n), tp), device_id_type=MESH,
            ).wait()
    for k in order:
        first[k].wait_send()
        second[k].wait_send()
        crossed[k].wait_send()


def combine(hidden, down_weight, n):
    capacity, width = hidden.shape[1] // n, down_weight.shape[1]
    vmem = pl.BlockSpec(memory_space=pltpu.VMEM)
    sems = pltpu.SemaphoreType.DMA
    blocks = pltpu.VMEM((n, capacity, width), jnp.bfloat16)
    return pl.pallas_call(
        functools.partial(combine_kernel, n),
        out_shape=jax.ShapeDtypeStruct((n, capacity, width), jnp.bfloat16),
        in_specs=[vmem, vmem],
        out_specs=vmem,
        scratch_shapes=[
            pltpu.VMEM((4, n, capacity, width), jnp.bfloat16),
            pltpu.VMEM((2, n, capacity, width), jnp.bfloat16),
            blocks, blocks, blocks]
        + [sems((n,))] * 8,
        compiler_params=pltpu.CompilerParams(collective_id=1, has_side_effects=True),
    )(hidden, down_weight)


def shards(
    queries,
    key_rows,
    value_rows,
    sink_logits,
    out_weight,
    mix_gain,
    moe_tokens,
    moe_gain,
    routes,
    route_weights,
    expert_gate,
    expert_up,
    expert_down,
):
    tok_rows, width = moe_tokens.shape
    top_count = routes.shape[1]
    experts = lax.axis_size("ep")
    capacity = tok_rows * top_count * 5 // (4 * experts)
    slots = capacity * experts

    normed = rms_scale(moe_tokens.astype(jnp.float32), moe_gain).astype(jnp.bfloat16)
    slot_place = slot_places(routes, experts, capacity)
    targets = jnp.arange(slots, dtype=jnp.int32)
    hits = (slot_place[None, :, :] == targets[:, None, None]).astype(jnp.float32)
    select_rows = jnp.sum(hits, axis=2).astype(jnp.bfloat16)
    outgoing = jnp.dot(select_rows, normed, preferred_element_type=jnp.float32)
    outgoing = outgoing.astype(jnp.bfloat16).reshape(experts, capacity, width)

    group_size = queries.shape[1] // HDIM
    q = jnp.transpose(queries.reshape(-1, group_size, HDIM), (1, 0, 2))
    q = jnp.pad(q, ((0, 0), (0, 0), (0, HDIM)))
    kv = jnp.concatenate([key_rows, value_rows], axis=1)
    weight = jnp.pad(out_weight.reshape(group_size, HDIM, width), ((0, 0), (HDIM, 0), (0, 0)))
    sinks = jnp.broadcast_to(sink_logits[:, None], (group_size, 128))
    slot_rows, mixed = dispatch(outgoing, q, kv, sinks, weight, mix_gain[None])

    slot_rows = slot_rows.reshape(4 * slots, width)
    gate_value = jnp.dot(slot_rows, expert_gate[0], preferred_element_type=jnp.float32)
    up_value = jnp.dot(slot_rows, expert_up[0], preferred_element_type=jnp.float32)
    hidden = (jax.nn.silu(gate_value) * up_value).astype(jnp.bfloat16)
    returned = combine(hidden.reshape(4, slots, -1), expert_down[0], experts).reshape(slots, width)

    spots = slot_place[:, :, None] == targets[None, None, :]
    spread = jnp.sum(jnp.where(spots, route_weights[:, :, None], 0.0), axis=1)
    high = spread.astype(jnp.bfloat16)
    low = (spread - high.astype(jnp.float32)).astype(jnp.bfloat16)
    combined = jnp.dot(high, returned, preferred_element_type=jnp.float32) + jnp.dot(
        low, returned, preferred_element_type=jnp.float32
    )
    return (mixed, combined.astype(jnp.bfloat16))


def solution(mesh):
    return jax.shard_map(
        shards,
        mesh=mesh,
        in_specs=(
            P("ep", "tp"),
            P("ep", "tp"),
            P("ep", "tp"),
            P("tp"),
            P("tp", None),
            P(),
            P(("ep", "tp"), None),
            P(),
            P(("ep", "tp"), None),
            P(("ep", "tp"), None),
            P("ep", None, "tp"),
            P("ep", None, "tp"),
            P("ep", "tp", None),
        ),
        out_specs=(P(("ep", "tp"), None), P(("ep", "tp"), None)),
        check_vma=False,
    )
```

```python
import functools

import jax
import jax.numpy as jnp
from jax import lax
from jax.experimental import pallas as pl
from jax.experimental.pallas import tpu as pltpu
from jax.sharding import PartitionSpec as P

HDIM = 64
WINDOW = 128
MESH = pl.DeviceIdType.MESH


norm_eps = 1e-06
masked_value = -1e30


def rms_scale(rows_in, gain):
    squares = jnp.mean(rows_in * rows_in, axis=-1, keepdims=True)
    return rows_in * lax.rsqrt(squares + norm_eps) * gain


def slot_places(route_rows, experts, capacity):
    tok_rows, top_count = route_rows.shape
    flat_routes = route_rows.reshape(tok_rows * top_count)
    onehot = (flat_routes[:, None] == jnp.arange(experts, dtype=jnp.int32)[None, :]).astype(jnp.int32)
    earlier = jnp.cumsum(onehot, axis=0) - onehot
    slot_rank = jnp.sum(earlier * onehot, axis=1)
    return (flat_routes * capacity + slot_rank).reshape(tok_rows, top_count)


def far_first(n):
    return sorted(range(1, n), key=lambda k: -min(k, n - k))


def places():
    ep, tp = lax.axis_index("ep"), lax.axis_index("tp")
    pair = tp + 1 - 2 * lax.rem(tp, 2)
    cross = lax.rem(tp + 2, 4)
    return ep, tp, pair, cross


def enter(n, ep, tp, pair, cross):
    barrier = pltpu.get_barrier_semaphore()
    for k in range(1, n):
        pl.semaphore_signal(barrier, inc=1, device_id=(lax.rem(ep + k, n), tp), device_id_type=MESH)
    for other in (pair, cross):
        pl.semaphore_signal(barrier, inc=1, device_id=(ep, other), device_id_type=MESH)
    pl.semaphore_wait(barrier, n + 1)


def send(src, dst, send_sem, recv_sem, where):
    copy = pltpu.make_async_remote_copy(
        src_ref=src, dst_ref=dst, send_sem=send_sem, recv_sem=recv_sem,
        device_id=where, device_id_type=MESH,
    )
    copy.start()
    return copy


def dispatch_kernel(
    n, out_ref, q_ref, kv_ref, sink_ref, w_ref, gain_ref,
    slots, mixed_ref,
    kv_prev, part, mix_in, mix_sum, mix_x,
    send_d, recv_d, send_p, recv_p, send_x, recv_x, send_q, recv_q, send_m, recv_m,
):
    ep, tp, pair, cross = places()
    diag = lax.rem(pair + 2, 4)
    enter(n, ep, tp, pair, cross)
    tok_rows = kv_ref.shape[0]
    group_size = q_ref.shape[0]
    copies = []
    halo = send(
        kv_ref.at[pl.ds(tok_rows - WINDOW, WINDOW)], kv_prev,
        send_m.at[0], recv_m.at[0], (lax.rem(ep + 1, n), tp),
    )
    order = far_first(n)[::-1]
    direct = {}
    own = out_ref.at[ep]
    crossed = {0: send(own, slots.at[2, 0], send_x.at[0], recv_x.at[0], (ep, cross))}
    for k in order:
        to = lax.rem(ep + k, n)
        direct[k] = send(out_ref.at[to], slots.at[0, k], send_d.at[k], recv_d.at[k], (to, tp))
    copies.append(send(own, slots.at[1, 0], send_p.at[0], recv_p.at[0], (ep, pair)))
    slots[0, 0] = out_ref[ep]

    halo.wait()
    rows = tok_rows + WINDOW
    kv = jnp.concatenate([kv_prev[...], kv_ref[...]], axis=0)
    row = lax.broadcasted_iota(jnp.int32, (tok_rows, rows), 0)
    col = lax.broadcasted_iota(jnp.int32, (tok_rows, rows), 1)
    distance = row - (col - WINDOW)
    key_pos = ep * tok_rows - WINDOW + col
    allowed = (distance >= 0) & (distance < WINDOW) & (key_pos >= 0)
    heads = []

    def attend(g):
        scores = lax.dot_general(
            q_ref[g], kv, (((1,), (1,)), ((), ())), preferred_element_type=jnp.float32
        ) * HDIM ** (-0.5)
        logits = jnp.where(allowed, scores, masked_value)
        sink = sink_ref[g : g + 1, 0:1]
        top = jnp.maximum(jnp.max(logits, axis=-1, keepdims=True), sink)
        exponent = jnp.exp(logits - top)
        denominator = jnp.sum(exponent, axis=-1, keepdims=True) + jnp.exp(sink - top)
        probs = (exponent / denominator).astype(jnp.bfloat16)
        heads.append(jnp.dot(probs, kv, preferred_element_type=jnp.float32).astype(jnp.bfloat16))

    block = tok_rows // 4
    mixing = {}

    def project():
        for b in range(4):
            total = None
            for g in range(group_size):
                term = jnp.dot(
                    heads[g][b * block : (b + 1) * block], w_ref[g], preferred_element_type=jnp.float32
                )
                total = term if total is None else total + term
            part[b] = total.astype(jnp.bfloat16)
        mixing["sum"] = send(part.at[diag], mix_in.at[1], send_m.at[1], recv_m.at[1], (ep, pair))
        mixing["own"] = send(part.at[pair], mix_in.at[0], send_m.at[2], recv_m.at[2], (ep, pair))

    def cross_part():
        mixing["sum"].wait()
        mix_sum[...] = (part[cross].astype(jnp.float32) + mix_in[1].astype(jnp.float32)).astype(jnp.bfloat16)
        mixing["x"] = send(mix_sum, mix_x, send_m.at[3], recv_m.at[3], (ep, cross))

    pieces = [functools.partial(attend, g) for g in range(group_size)] + [project, cross_part]

    pending = [0]
    for k in order:
        direct[k].wait_recv()
        crossed[k] = send(slots.at[0, k], slots.at[2, k], send_x.at[k], recv_x.at[k], (ep, cross))
        copies.append(send(slots.at[0, k], slots.at[1, k], send_p.at[k], recv_p.at[k], (ep, pair)))
        pending.append(k)
        if pieces:
            pieces.pop(0)()
    for piece in pieces:
        piece()
    diagonal = []
    for i, k in enumerate(pending):
        crossed[k].wait_recv()
        diagonal.append(send(slots.at[2, k], slots.at[3, k], send_q.at[k], recv_q.at[k], (ep, pair)))
        if i == 1 or n == 1:
            mixing["own"].wait()
            mixing["x"].wait()
            projected = (
                part[tp].astype(jnp.float32) + mix_in[0].astype(jnp.float32) + mix_x[...].astype(jnp.float32)
            )
            mixed_ref[...] = rms_scale(projected, gain_ref[...]).astype(jnp.bfloat16)
    for copy in copies + diagonal:
        copy.wait()
    for k in order:
        direct[k].wait_send()
    for k in pending:
        crossed[k].wait_send()


def dispatch(outgoing, queries, kv, sinks, weight, gain):
    n, capacity, width = outgoing.shape
    tok_rows = kv.shape[0]
    block = tok_rows // 4
    vmem = pl.BlockSpec(memory_space=pltpu.VMEM)
    sems = pltpu.SemaphoreType.DMA
    return pl.pallas_call(
        functools.partial(dispatch_kernel, n),
        out_shape=(
            jax.ShapeDtypeStruct((4, n, capacity, width), jnp.bfloat16),
            jax.ShapeDtypeStruct((block, width), jnp.bfloat16),
        ),
        in_specs=[vmem] * 6,
        out_specs=(vmem, vmem),
        scratch_shapes=[
            pltpu.VMEM((WINDOW, kv.shape[1]), jnp.bfloat16),
            pltpu.VMEM((4, block, width), jnp.bfloat16),
            pltpu.VMEM((2, block, width), jnp.bfloat16),
            pltpu.VMEM((block, width), jnp.bfloat16),
            pltpu.VMEM((block, width), jnp.bfloat16),
        ]
        + [sems((n,))] * 8
        + [sems((4,))] * 2,
        compiler_params=pltpu.CompilerParams(collective_id=0, has_side_effects=True),
    )(outgoing, queries, kv, sinks, weight, gain)


def combine_kernel(
    n, h_ref, down_ref, ret, y_ref, pair_in, cross_out, cross_in, back_out,
    send_a, recv_a, send_b, recv_b, send_x, recv_x, send_r, recv_r,
):
    ep, tp, pair, cross = places()
    enter(n, ep, tp, pair, cross)
    order = far_first(n) + [0]
    capacity, width = ret.shape[1:]
    tile = width // 4
    first, second, crossed, back = {}, {}, {}, {}

    def down(r):
        for c in range(0, width, tile):
            product = jnp.dot(
                h_ref[r], down_ref[:, c : c + tile], preferred_element_type=jnp.float32
            ).astype(jnp.bfloat16)
            for k in range(n):
                y_ref[r, k, :, c : c + tile] = product[k * capacity : (k + 1) * capacity]

    down(3)
    for k in order:
        first[k] = send(y_ref.at[3, k], pair_in.at[1, k], send_a.at[k], recv_a.at[k], (ep, pair))
    down(2)
    for k in order:
        first[k].wait_recv()
        cross_out[k] = (
            y_ref[2, k].astype(jnp.float32) + pair_in[1, k].astype(jnp.float32)
        ).astype(jnp.bfloat16)
        crossed[k] = send(cross_out.at[k], cross_in.at[k], send_x.at[k], recv_x.at[k], (ep, cross))
    down(1)
    for k in order:
        second[k] = send(y_ref.at[1, k], pair_in.at[0, k], send_b.at[k], recv_b.at[k], (ep, pair))
    down(0)
    for k in order:
        second[k].wait_recv()
        crossed[k].wait_recv()
        total = (
            y_ref[0, k].astype(jnp.float32)
            + pair_in[0, k].astype(jnp.float32)
            + cross_in[k].astype(jnp.float32)
        ).astype(jnp.bfloat16)
        if k == 0:
            ret[ep] = total
        else:
            back_out[k] = total
            to = lax.rem(ep + n - k, n)
            back[k] = send(back_out.at[k], ret.at[ep], send_r.at[k], recv_r.at[k], (to, tp))
    for k in order:
        if k:
            pltpu.make_async_remote_copy(
                src_ref=back_out.at[k], dst_ref=ret.at[lax.rem(ep + k, n)],
                send_sem=send_r.at[k], recv_sem=recv_r.at[k],
                device_id=(lax.rem(ep + n - k, n), tp), device_id_type=MESH,
            ).wait()
    for k in order:
        first[k].wait_send()
        second[k].wait_send()
        crossed[k].wait_send()


def combine(hidden, down_weight, n):
    capacity, width = hidden.shape[1] // n, down_weight.shape[1]
    vmem = pl.BlockSpec(memory_space=pltpu.VMEM)
    sems = pltpu.SemaphoreType.DMA
    blocks = pltpu.VMEM((n, capacity, width), jnp.bfloat16)
    return pl.pallas_call(
        functools.partial(combine_kernel, n),
        out_shape=jax.ShapeDtypeStruct((n, capacity, width), jnp.bfloat16),
        in_specs=[vmem, vmem],
        out_specs=vmem,
        scratch_shapes=[
            pltpu.VMEM((4, n, capacity, width), jnp.bfloat16),
            pltpu.VMEM((2, n, capacity, width), jnp.bfloat16),
            blocks, blocks, blocks]
        + [sems((n,))] * 8,
        compiler_params=pltpu.CompilerParams(collective_id=1, has_side_effects=True),
    )(hidden, down_weight)


def shards(
    queries,
    key_rows,
    value_rows,
    sink_logits,
    out_weight,
    mix_gain,
    moe_tokens,
    moe_gain,
    routes,
    route_weights,
    expert_gate,
    expert_up,
    expert_down,
):
    tok_rows, width = moe_tokens.shape
    top_count = routes.shape[1]
    experts = lax.axis_size("ep")
    capacity = tok_rows * top_count * 5 // (4 * experts)
    slots = capacity * experts

    normed = rms_scale(moe_tokens.astype(jnp.float32), moe_gain).astype(jnp.bfloat16)
    slot_place = slot_places(routes, experts, capacity)
    targets = jnp.arange(slots, dtype=jnp.int32)
    hits = (slot_place[None, :, :] == targets[:, None, None]).astype(jnp.float32)
    select_rows = jnp.sum(hits, axis=2).astype(jnp.bfloat16)
    outgoing = jnp.dot(select_rows, normed, preferred_element_type=jnp.float32)
    outgoing = outgoing.astype(jnp.bfloat16).reshape(experts, capacity, width)

    group_size = queries.shape[1] // HDIM
    q = jnp.transpose(queries.reshape(-1, group_size, HDIM), (1, 0, 2))
    q = jnp.pad(q, ((0, 0), (0, 0), (0, HDIM)))
    kv = jnp.concatenate([key_rows, value_rows], axis=1)
    weight = jnp.pad(out_weight.reshape(group_size, HDIM, width), ((0, 0), (HDIM, 0), (0, 0)))
    sinks = jnp.broadcast_to(sink_logits[:, None], (group_size, 128))
    slot_rows, mixed = dispatch(outgoing, q, kv, sinks, weight, mix_gain[None])

    slot_rows = slot_rows.reshape(4 * slots, width)
    gate_value = jnp.dot(slot_rows, expert_gate[0], preferred_element_type=jnp.float32)
    up_value = jnp.dot(slot_rows, expert_up[0], preferred_element_type=jnp.float32)
    hidden = (jax.nn.silu(gate_value) * up_value).astype(jnp.bfloat16)
    returned = combine(hidden.reshape(4, slots, -1), expert_down[0], experts).reshape(slots, width)

    spots = slot_place[:, :, None] == targets[None, None, :]
    spread = jnp.sum(jnp.where(spots, route_weights[:, :, None], 0.0), axis=1)
    high = spread.astype(jnp.bfloat16)
    low = (spread - high.astype(jnp.float32)).astype(jnp.bfloat16)
    combined = jnp.dot(high, returned, preferred_element_type=jnp.float32) + jnp.dot(
        low, returned, preferred_element_type=jnp.float32
    )
    return (mixed, combined.astype(jnp.bfloat16))


def solution(mesh):
    return jax.shard_map(
        shards,
        mesh=mesh,
        in_specs=(
            P("ep", "tp"),
            P("ep", "tp"),
            P("ep", "tp"),
            P("tp"),
            P("tp", None),
            P(),
            P(("ep", "tp"), None),
            P(),
            P(("ep", "tp"), None),
            P(("ep", "tp"), None),
            P("ep", None, "tp"),
            P("ep", None, "tp"),
            P("ep", "tp", None),
        ),
        out_specs=(P(("ep", "tp"), None), P(("ep", "tp"), None)),
        check_vma=False,
    )
```
